32 devices in a mesh: grp: 2 (over y), ra: 4 (over z), cb: 4 (over x, core).
Axes of the slice: x: 2, y: 2, z: 4, core: 2. Of those that a mesh axis runs over, the one named last changes fastest.
Arguments:
- residual: bfloat16 [512, 4096], P('grp', 'ra'), parts along dimension 0, may hold values from -6 to 6
- gain_first: bfloat16 [4096], P('ra'), may hold values from 0.099609375 to 1.8984375
- gate_first: bfloat16 [4096, 11264], P('ra', 'cb'), may hold values from -0.09375 to 0.09375
- up_first: bfloat16 [4096, 11264], P('ra', 'cb'), may hold values from -0.09375 to 0.09375
- down_first: bfloat16 [11264, 4096], P('cb', 'ra'), may hold values from -0.078125 to 0.078125
- gain_second: bfloat16 [4096], P('ra'), may hold values from 0.099609375 to 1.8984375
- gate_second: bfloat16 [4096, 11264], P('ra', 'cb'), may hold values from -0.09375 to 0.09375
- up_second: bfloat16 [4096, 11264], P('ra', 'cb'), may hold values from -0.09375 to 0.09375
- down_second: bfloat16 [11264, 4096], P('cb', 'ra'), may hold values from -0.078125 to 0.078125
Outputs:
- updated: bfloat16 [512, 4096], P('grp', 'ra'), parts along dimension 0
The draws below stay inside these ranges and needn't reach their ends.
There are 2 independent parts, one for each index of `grp`. The reference program is written for one: setup_inputs(seed, part) draws one part's arguments, and reference() takes and returns one part's arrays. A program takes and returns all parts, laid end to end along the dimension named above; an argument that names none is the same for every part. Nothing has to cross between parts.
All inputs are finite; a program needn't handle non-finite values.
Results may differ from the reference program's by a relative error of at most 0.0071.
Values may be sent and summed in bfloat16 or wider, within the bound.
A program may use at most 128 MiB of HBM per device.

```python
import jax
import jax.numpy as jnp
from jax import lax

D = 4096
FF = 11264
TOK = 256


def draw_residual(key, part):
    first, second, third = jax.random.split(jax.random.fold_in(key, 11), 3)
    rows = jnp.exp(jax.random.uniform(first, (TOK, 1), jnp.float32, jnp.log(0.25), jnp.log(2.5)))
    ramp = jnp.exp(jnp.linspace(jnp.log(0.5), jnp.log(2.0), D)).astype(jnp.float32)
    columns = ramp[None, :] * jnp.exp(jax.random.uniform(third, (1, D), jnp.float32, -0.3, 0.3))
    base = jnp.clip(jax.random.normal(second, (TOK, D), jnp.float32), -4.0, 4.0)
    return jnp.clip(0.4 * rows * columns * base, -6.0, 6.0).astype(jnp.bfloat16)


def spiked(values, stream_key, source, target, blocks, factor):
    def block_of(position):
        return (jnp.arange(values.shape[position]) // (values.shape[position] // blocks)).reshape((-1,) + (1,) * (values.ndim - 1 - position))

    near = jax.random.permutation(stream_key, blocks)[block_of(target)]
    far = (block_of(target) + blocks // 2) % blocks
    return jnp.where((block_of(source) == near) | (block_of(source) == far), factor * values, values)


def level_of(own_key, extent, cuts, smallest, high):
    def one(position, shards_of):
        heights = jax.random.uniform(jax.random.fold_in(jax.random.fold_in(own_key, 6), position), (shards_of,), jnp.float32, smallest / len(cuts), high / len(cuts))
        return jnp.repeat(jnp.exp(heights), extent[position] // shards_of).reshape((-1,) + (1,) * (len(extent) - position - 1))

    level = one(*cuts[0])
    for cut in cuts[1:]:
        level = level * one(*cut)
    return level


def bell_draw(stream_key, extent, width, reach, pieces=(), kind=jnp.bfloat16):
    level = level_of(stream_key, extent, pieces, -0.22, 0.18) if pieces else 1.0
    array = jax.random.normal(stream_key, extent, jnp.float32) * width * level
    return jnp.minimum(jnp.maximum(array, -reach), reach).astype(kind)


def heavy_noise(own_key, extent, width, bound, shards, heavy, held_as=jnp.bfloat16):
    drawn = width * jax.random.normal(own_key, extent, jnp.float32)
    if shards:
        drawn = drawn * level_of(own_key, extent, shards, -0.22, 0.18)
    return jnp.clip(spiked(drawn, jax.random.fold_in(own_key, 3), *heavy), -bound, bound).astype(held_as)


def setup_inputs(seed: int = 0, part: int = 0) -> dict:
    arg_keys = jax.random.split(jax.random.key(seed), 10)
    part_splits = jax.random.split(jax.random.fold_in(arg_keys[9], part), 10)
    residual = draw_residual(jax.random.fold_in(jax.random.fold_in(arg_keys[9], part), 71), part)
    gain_first = jnp.clip(1.0 + 0.18 * jax.random.normal(arg_keys[1], (D,), jnp.float32), 0.099609375, 1.8984375).astype(jnp.bfloat16)
    gate_first = bell_draw(arg_keys[2], (D, FF), D ** -0.5, 0.09375, ((0, 4), (1, 4)))
    up_first = bell_draw(arg_keys[3], (D, FF), D ** -0.5, 0.09375, ((0, 4), (1, 4)))
    down_first = heavy_noise(arg_keys[4], (FF, D), FF ** -0.5, 0.078125, ((0, 4), (1, 4)), (0, 1, 4, 2.0))
    gain_second = jnp.clip(1.0 + 0.18 * jax.random.normal(arg_keys[5], (D,), jnp.float32), 0.099609375, 1.8984375).astype(jnp.bfloat16)
    gate_second = bell_draw(arg_keys[6], (D, FF), D ** -0.5, 0.09375, ((0, 4), (1, 4)))
    up_second = bell_draw(arg_keys[7], (D, FF), D ** -0.5, 0.09375, ((0, 4), (1, 4)))
    down_second = heavy_noise(arg_keys[8], (FF, D), FF ** -0.5, 0.078125, ((0, 4), (1, 4)), (0, 1, 4, 2.0))
    return dict(residual=residual, gain_first=gain_first, gate_first=gate_first, up_first=up_first, down_first=down_first, gain_second=gain_second, gate_second=gate_second, up_second=up_second, down_second=down_second)


epsilon = 1e-06

def half_step(stream, gain, w_gate, w_up, w_down):
    values = stream.astype(jnp.float32)
    scale = lax.rsqrt(lax.optimization_barrier(jnp.mean(values * values, axis=1, keepdims=True)) + epsilon)
    normed = (values * gain.astype(jnp.float32)).astype(jnp.bfloat16)
    gate = scale * jnp.dot(normed, w_gate, preferred_element_type=jnp.float32)
    upward = scale * jnp.dot(normed, w_up, preferred_element_type=jnp.float32)
    hidden = (jax.nn.silu(gate) * upward).astype(jnp.bfloat16)
    branch = jnp.dot(hidden, w_down, preferred_element_type=jnp.float32)
    return (values + 0.5 * branch).astype(jnp.bfloat16)

def reference(residual, gain_first, gate_first, up_first, down_first, gain_second, gate_second, up_second, down_second):
    middle = half_step(residual, gain_first, gate_first, up_first, down_first)
    return half_step(middle, gain_second, gate_second, up_second, down_second)
```

```python
import functools

import jax
import jax.numpy as jnp
from jax import lax
from jax.experimental import pallas as pl
from jax.experimental.pallas import tpu as pltpu
from jax.sharding import PartitionSpec as P

MESH = pl.DeviceIdType.MESH
LANES = 128
epsilon = 1e-06

HOP = 3
REDUCE = 4
SPREAD = 4


def kernel(
    cfg,
    residual,
    gain_first,
    gain_second,
    gate_first,
    up_first,
    down_first,
    gate_second,
    up_second,
    down_second,
    out,
    w_in,
    w_down,
    normed,
    own,
    part_out,
    part_in,
    hidden,
    total,
    rs_own,
    rs_out,
    rs_in,
    merged,
    sq_own,
    sq_out,
    sq_in,
    scale,
    w_sem,
    part_send,
    part_recv,
    hid_send,
    hid_recv,
    sq_send,
    sq_recv,
    rs_send,
    rs_recv,
    ag_send,
    ag_recv,
):
    R, C, blocks, pieces, width, half_rows, gap, model = cfg
    rows = 2 * half_rows
    per_phase = blocks * pieces
    count = 2 * per_phase
    r = lax.axis_index("ra")
    c = lax.axis_index("cb")

    gates, ups, downs = (gate_first, gate_second), (up_first, up_second), (down_first, down_second)

    def weight_copy(phase, p, which):
        span = pl.ds(p * width, width)
        if which == 2:
            return pltpu.make_async_copy(
                downs[phase].at[span, :], w_down.at[phase, p], w_sem.at[phase, 2, p]
            )
        source = (gates, ups)[which][phase]
        return pltpu.make_async_copy(
            source.at[:, span], w_in.at[phase, p, which], w_sem.at[phase, which, p]
        )

    for phase in range(2):
        for p in range(pieces):
            weight_copy(phase, p, 0).start()
            weight_copy(phase, p, 1).start()
        for p in range(pieces):
            weight_copy(phase, p, 2).start()

    barrier = pltpu.get_barrier_semaphore()

    @pl.when(r > 0)
    def _():
        pl.semaphore_signal(barrier, inc=1, device_id={"ra": r - 1}, device_id_type=MESH)

    @pl.when(r < R - 1)
    def _():
        pl.semaphore_signal(barrier, inc=1, device_id={"ra": r + 1}, device_id_type=MESH)

    for k in range(1, C):
        pl.semaphore_signal(
            barrier, inc=1, device_id={"cb": lax.rem(c + k, C)}, device_id_type=MESH
        )

    def prepare(phase, block, stream, gain_ref):
        values = stream.astype(jnp.float32)
        square = jnp.sum(values * values, axis=1, keepdims=True)
        normed[phase, block] = (values * gain_ref[...].astype(jnp.float32)).astype(jnp.bfloat16)
        sq_own[phase, block] = jnp.broadcast_to(square, (rows, LANES)).reshape(2, half_rows, LANES)

    def first(block, carry):
        prepare(0, block, residual[block].reshape(rows, -1), gain_first)
        return carry

    lax.fori_loop(0, blocks, first, 0)

    near = jnp.where(r > 0, 1, 0) + jnp.where(r < R - 1, 1, 0)
    pl.semaphore_wait(barrier, C - 1 + near)

    place = (r, R - 1 - r)
    onward = (r + 1, r - 1)
    back = (r - 1, r + 1)

    def part_copy(d, i):
        return pltpu.make_async_remote_copy(
            src_ref=part_out.at[i, d],
            dst_ref=part_in.at[i, d],
            send_sem=part_send.at[d, i],
            recv_sem=part_recv.at[d, i],
            device_id={"ra": onward[d]},
            device_id_type=MESH,
        )

    def square_copy(d, pb):
        return pltpu.make_async_remote_copy(
            src_ref=sq_out.at[pb, d],
            dst_ref=sq_in.at[pb, d],
            send_sem=sq_send.at[d, pb],
            recv_sem=sq_recv.at[d, pb],
            device_id={"ra": onward[d]},
            device_id_type=MESH,
        )

    def hidden_copy(d, i):
        return pltpu.make_async_remote_copy(
            src_ref=hidden.at[i, d],
            dst_ref=hidden.at[i, d],
            send_sem=hid_send.at[d, i],
            recv_sem=hid_recv.at[d, i],
            device_id={"ra": back[d]},
            device_id_type=MESH,
        )

    def reduce_copy(pb, k):
        peer = lax.rem(c + k, C)
        return pltpu.make_async_remote_copy(
            src_ref=rs_out.at[pb, peer],
            dst_ref=rs_in.at[pb, k - 1],
            send_sem=rs_send.at[pb, k - 1],
            recv_sem=rs_recv.at[pb, k - 1],
            device_id={"cb": peer},
            device_id_type=MESH,
        )

    def spread_copy(pb, k):
        return pltpu.make_async_remote_copy(
            src_ref=merged.at[pb, c],
            dst_ref=merged.at[pb, c],
            send_sem=ag_send.at[pb, k - 1],
            recv_sem=ag_recv.at[pb, k - 1],
            device_id={"cb": lax.rem(c + k, C)},
            device_id_type=MESH,
        )

    def at_step(slot, body):
        early = (slot >= 0) & (slot < per_phase)
        late = (slot >= per_phase + gap) & (slot < count + gap)

        @pl.when(early | late)
        def _():
            phase = jnp.where(late, 1, 0)
            i = slot - phase * gap
            local = i - phase * per_phase
            block = lax.div(local, pieces)
            p = lax.rem(local, pieces)
            body(i, phase, block, p)

    def both_phases(phase, body):
        for static in range(2):

            @pl.when(phase == static)
            def _():
                body(static)

    def project(i, phase, block, p):
        @pl.when(block == 0)
        def _():
            def waits(static):
                weight_copy(static, p, 0).wait()
                weight_copy(static, p, 1).wait()

            both_phases(phase, waits)

        slot = i - phase * per_phase
        x = normed[phase, block]
        for which in range(2):
            product = jnp.dot(x, w_in[phase, p, which], preferred_element_type=jnp.float32)
            own[slot, 0, which] = product[:half_rows]
            own[slot, 1, which] = product[half_rows:]

    def forward(d):
        def body(i, phase, block, p):
            slot = i - phase * per_phase
            pb = phase * blocks + block

            @pl.when(place[d] == 0)
            def _():
                part_out[i, d] = own[slot, d].astype(jnp.bfloat16)
                part_copy(d, i).start()

                @pl.when(p == 0)
                def _():
                    sq_out[pb, d] = sq_own[phase, block, d]
                    square_copy(d, pb).start()

            @pl.when((place[d] > 0) & (place[d] < R - 1))
            def _():
                part_copy(d, i).wait_recv()
                part_out[i, d] = (own[slot, d] + part_in[i, d].astype(jnp.float32)).astype(
                    jnp.bfloat16
                )
                part_copy(d, i).start()

                @pl.when(p == 0)
                def _():
                    square_copy(d, pb).wait_recv()
                    sq_out[pb, d] = sq_own[phase, block, d] + sq_in[pb, d]
                    square_copy(d, pb).start()

            @pl.when(place[d] == R - 1)
            def _():
                @pl.when(p == 0)
                def _():
                    square_copy(d, pb).wait_recv()
                    mean = (sq_own[phase, block, d] + sq_in[pb, d]) / model
                    scale[d] = lax.rsqrt(mean + epsilon)

                part_copy(d, i).wait_recv()
                factor = scale[d][:, :1]
                gate = (own[slot, d, 0] + part_in[i, d, 0].astype(jnp.float32)) * factor
                up = (own[slot, d, 1] + part_in[i, d, 1].astype(jnp.float32)) * factor
                hidden[i, d] = (gate / (1.0 + jnp.exp(-gate)) * up).astype(jnp.bfloat16)
                hidden_copy(d, i).start()

        return body

    def pass_back(d):
        def body(i, phase, block, p):
            @pl.when(place[d] < R - 1)
            def _():
                hidden_copy(d, i).wait_recv()

                @pl.when(place[d] > 0)
                def _():
                    hidden_copy(d, i).start()

        return body

    def down(i, phase, block, p):
        @pl.when(block == 0)
        def _():
            both_phases(phase, lambda static: weight_copy(static, p, 2).wait())

        product = jnp.dot(
            hidden[i].reshape(rows, width), w_down[phase, p], preferred_element_type=jnp.float32
        ).reshape(total.shape)

        @pl.when(p == 0)
        def _():
            total[...] = product

        @pl.when(p > 0)
        def _():
            total[...] += product

        @pl.when(p == pieces - 1)
        def _():
            pb = phase * blocks + block
            rs_own[pb] = total[c]
            rs_out[pb] = total[...].astype(jnp.bfloat16)
            for k in range(1, C):
                reduce_copy(pb, k).start()

    def reduce(i, phase, block, p):
        @pl.when(p == pieces - 1)
        def _():
            pb = phase * blocks + block
            branch = rs_own[pb]
            for k in range(1, C):
                reduce_copy(pb, k).wait_recv()
                branch = branch + rs_in[pb, k - 1].astype(jnp.float32)

            @pl.when(phase == 0)
            def _():
                values = residual[block, c].astype(jnp.float32)
                merged[pb, c] = (values + 0.5 * branch).astype(jnp.bfloat16)

            @pl.when(phase == 1)
            def _():
                values = merged[block, c].astype(jnp.float32)
                merged[pb, c] = (values + 0.5 * branch).astype(jnp.bfloat16)

            for k in range(1, C):
                spread_copy(pb, k).start()

    def spread(i, phase, block, p):
        @pl.when(p == pieces - 1)
        def _():
            pb = phase * blocks + block
            for k in range(1, C):
                spread_copy(pb, k).wait_recv()

            @pl.when(phase == 0)
            def _():
                prepare(1, block, merged[pb].reshape(rows, -1), gain_second)

            @pl.when(phase == 1)
            def _():
                out[block] = merged[pb]

    reach = HOP * (R - 1)
    end = 2 * reach

    def step(s, carry):
        at_step(s - end - REDUCE - SPREAD, spread)
        at_step(s, project)
        for d in range(2):
            at_step(s - HOP * place[d], forward(d))
        for d in range(2):
            at_step(s - reach - HOP * (R - 1 - place[d]), pass_back(d))
        at_step(s - end, down)
        at_step(s - end - REDUCE, reduce)
        return carry

    lax.fori_loop(0, count + gap + end + REDUCE + SPREAD, step, 0)

    def finish(i, carry):
        for d in range(2):

            @pl.when(place[d] < R - 1)
            def _():
                part_copy(d, i).wait_send()

            @pl.when(place[d] > 0)
            def _():
                hidden_copy(d, i).wait_send()

        return carry

    lax.fori_loop(0, count, finish, 0)

    def finish_block(pb, carry):
        for d in range(2):

            @pl.when(place[d] < R - 1)
            def _():
                square_copy(d, pb).wait_send()

        for k in range(1, C):
            reduce_copy(pb, k).wait_send()
            spread_copy(pb, k).wait_send()
        return carry

    lax.fori_loop(0, 2 * blocks, finish_block, 0)


def solution(mesh):
    R, C = mesh.shape["ra"], mesh.shape["cb"]

    def per_device(
        residual,
        gain_first,
        gate_first,
        up_first,
        down_first,
        gain_second,
        gate_second,
        up_second,
        down_second,
    ):
        tokens, depth = residual.shape
        units = gate_first.shape[1]
        blocks = max(1, min(4, tokens // (16 * C)))
        width = 2 * LANES if units % (2 * LANES) == 0 else units
        pieces = units // width
        rows = tokens // blocks
        half_rows = rows // 2
        share = rows // C
        count = 2 * blocks * pieces
        end = 2 * HOP * (R - 1) + REDUCE + SPREAD
        gap = max(0, pieces - 1 + end - blocks * pieces)
        bf16, f32 = jnp.bfloat16, jnp.float32
        vmem = functools.partial(pl.BlockSpec, memory_space=pltpu.VMEM)
        hbm = functools.partial(pl.BlockSpec, memory_space=pl.ANY)
        pbs = 2 * blocks
        dma = pltpu.SemaphoreType.DMA
        result = pl.pallas_call(
            functools.partial(
                kernel, (R, C, blocks, pieces, width, half_rows, gap, float(depth * R))
            ),
            out_shape=jax.ShapeDtypeStruct((blocks, C, share, depth), bf16),
            in_specs=[vmem()] * 3 + [hbm()] * 6,
            out_specs=vmem(),
            scratch_shapes=[
                pltpu.VMEM((2, pieces, 2, depth, width), bf16),
                pltpu.VMEM((2, pieces, width, depth), bf16),
                pltpu.VMEM((2, blocks, rows, depth), bf16),
                pltpu.VMEM((blocks * pieces, 2, 2, half_rows, width), f32),
                pltpu.VMEM((count, 2, 2, half_rows, width), bf16),
                pltpu.VMEM((count, 2, 2, half_rows, width), bf16),
                pltpu.VMEM((count, 2, half_rows, width), bf16),
                pltpu.VMEM((C, share, depth), f32),
                pltpu.VMEM((pbs, share, depth), f32),
                pltpu.VMEM((pbs, C, share, depth), bf16),
                pltpu.VMEM((pbs, C - 1, share, depth), bf16),
                pltpu.VMEM((pbs, C, share, depth), bf16),
                pltpu.VMEM((2, blocks, 2, half_rows, LANES), f32),
                pltpu.VMEM((pbs, 2, half_rows, LANES), f32),
                pltpu.VMEM((pbs, 2, half_rows, LANES), f32),
                pltpu.VMEM((2, half_rows, LANES), f32),
                dma((2, 3, pieces)),
                dma((2, count)),
                dma((2, count)),
                dma((2, count)),
                dma((2, count)),
                dma((2, pbs)),
                dma((2, pbs)),
                dma((pbs, C - 1)),
                dma((pbs, C - 1)),
                dma((pbs, C - 1)),
                dma((pbs, C - 1)),
            ],
            compiler_params=pltpu.CompilerParams(
                collective_id=0, has_side_effects=True, vmem_limit_bytes=67043328
            ),
        )(
            residual.reshape(blocks, C, share, depth),
            gain_first.reshape(1, depth),
            gain_second.reshape(1, depth),
            gate_first,
            up_first,
            down_first,
            gate_second,
            up_second,
            down_second,
        )
        return result.reshape(tokens, depth)

    in_specs = (
        P("grp", "ra"),
        P("ra"),
        P("ra", "cb"),
        P("ra", "cb"),
        P("cb", "ra"),
        P("ra"),
        P("ra", "cb"),
        P("ra", "cb"),
        P("cb", "ra"),
    )
    return jax.shard_map(
        per_device, mesh=mesh, in_specs=in_specs, out_specs=P("grp", "ra"), check_vma=False
    )
```

```python
import functools

import jax
import jax.numpy as jnp
from jax import lax
from jax.experimental import pallas as pl
from jax.experimental.pallas import tpu as pltpu
from jax.sharding import PartitionSpec as P

MESH = pl.DeviceIdType.MESH
LANES = 128
epsilon = 1e-06

HOP = 4
REDUCE = 4
SPREAD = 4
TILE = 8


def kernel(
    cfg,
    residual,
    gain_first,
    gain_second,
    gate_first,
    up_first,
    down_first,
    gate_second,
    up_second,
    down_second,
    out,
    w_in,
    w_down,
    normed,
    own,
    part_out,
    part_in,
    hidden,
    total,
    rs_own,
    rs_out,
    rs_in,
    merged,
    sq_own,
    sq_out,
    sq_in,
    scale,
    w_sem,
    part_send,
    part_recv,
    hid_send,
    hid_recv,
    sq_send,
    sq_recv,
    rs_send,
    rs_recv,
    ag_send,
    ag_recv,
):
    R, C, blocks, pieces, width, half_rows, gap, model = cfg
    rows = 2 * half_rows
    per_phase = blocks * pieces
    count = 2 * per_phase
    r = lax.axis_index("ra")
    c = lax.axis_index("cb")

    gates, ups, downs = (gate_first, gate_second), (up_first, up_second), (down_first, down_second)

    def weight_copy(phase, p, which):
        span = pl.ds(p * width, width)
        if which == 2:
            return pltpu.make_async_copy(
                downs[phase].at[span, :], w_down.at[phase, p], w_sem.at[phase, 2, p]
            )
        source = (gates, ups)[which][phase]
        return pltpu.make_async_copy(
            source.at[:, span], w_in.at[phase, p, which], w_sem.at[phase, which, p]
        )

    for p in range(pieces):
        weight_copy(0, p, 0).start()
        weight_copy(0, p, 1).start()

    def load_rest(s):
        @pl.when(s == 2)
        def _():
            for p in range(pieces):
                weight_copy(0, p, 2).start()

        @pl.when(s == 6)
        def _():
            for p in range(pieces):
                weight_copy(1, p, 0).start()
                weight_copy(1, p, 1).start()
            for p in range(pieces):
                weight_copy(1, p, 2).start()

    barrier = pltpu.get_barrier_semaphore()

    @pl.when(r > 0)
    def _():
        pl.semaphore_signal(barrier, inc=1, device_id={"ra": r - 1}, device_id_type=MESH)

    @pl.when(r < R - 1)
    def _():
        pl.semaphore_signal(barrier, inc=1, device_id={"ra": r + 1}, device_id_type=MESH)

    for k in range(1, C):
        pl.semaphore_signal(
            barrier, inc=1, device_id={"cb": lax.rem(c + k, C)}, device_id_type=MESH
        )

    def diagonal():
        shape = (half_rows, half_rows)
        return lax.broadcasted_iota(jnp.int32, shape, 0) == lax.broadcasted_iota(jnp.int32, shape, 1)

    def prepare(phase, block, stream, gain_ref):
        values = stream.astype(jnp.float32)
        square = jnp.sum(values * values, axis=1, keepdims=True)
        normed[phase, block] = (values * gain_ref[...].astype(jnp.float32)).astype(jnp.bfloat16)
        for d in range(2):
            column = square[d * half_rows : (d + 1) * half_rows]
            line = jnp.sum(jnp.where(diagonal(), column, 0.0), axis=0, keepdims=True)
            sq_own[phase, block, d] = jnp.broadcast_to(line, (TILE, half_rows))

    def first(block):
        prepare(0, block, residual[block].reshape(rows, -1), gain_first)

    first(0)

    near = jnp.where(r > 0, 1, 0) + jnp.where(r < R - 1, 1, 0)
    pl.semaphore_wait(barrier, C - 1 + near)

    place = (r, R - 1 - r)
    onward = (r + 1, r - 1)
    back = (r - 1, r + 1)

    def part_copy(d, i):
        return pltpu.make_async_remote_copy(
            src_ref=part_out.at[i, d],
            dst_ref=part_in.at[i, d],
            send_sem=part_send.at[d, i],
            recv_sem=part_recv.at[d, i],
            device_id={"ra": onward[d]},
            device_id_type=MESH,
        )

    def square_copy(d, pb):
        return pltpu.make_async_remote_copy(
            src_ref=sq_out.at[pb, d],
            dst_ref=sq_in.at[pb, d],
            send_sem=sq_send.at[d, pb],
            recv_sem=sq_recv.at[d, pb],
            device_id={"ra": onward[d]},
            device_id_type=MESH,
        )

    def hidden_copy(d, i):
        return pltpu.make_async_remote_copy(
            src_ref=hidden.at[i, d],
            dst_ref=hidden.at[i, d],
            send_sem=hid_send.at[d, i],
            recv_sem=hid_recv.at[d, i],
            device_id={"ra": back[d]},
            device_id_type=MESH,
        )

    def reduce_copy(pb, k):
        peer = lax.rem(c + k, C)
        return pltpu.make_async_remote_copy(
            src_ref=rs_out.at[pb, peer],
            dst_ref=rs_in.at[pb, k - 1],
            send_sem=rs_send.at[pb, k - 1],
            recv_sem=rs_recv.at[pb, k - 1],
            device_id={"cb": peer},
            device_id_type=MESH,
        )

    def spread_copy(pb, k):
        return pltpu.make_async_remote_copy(
            src_ref=merged.at[pb, c],
            dst_ref=merged.at[pb, c],
            send_sem=ag_send.at[pb, k - 1],
            recv_sem=ag_recv.at[pb, k - 1],
            device_id={"cb": lax.rem(c + k, C)},
            device_id_type=MESH,
        )

    def at_step(slot, body):
        early = (slot >= 0) & (slot < per_phase)
        late = (slot >= per_phase + gap) & (slot < count + gap)

        @pl.when(early | late)
        def _():
            phase = jnp.where(late, 1, 0)
            i = slot - phase * gap
            local = i - phase * per_phase
            block = lax.div(local, pieces)
            p = lax.rem(local, pieces)
            body(i, phase, block, p)

    def both_phases(phase, body):
        for static in range(2):

            @pl.when(phase == static)
            def _():
                body(static)

    def project(i, phase, block, p):
        @pl.when(block == 0)
        def _():
            def waits(static):
                weight_copy(static, p, 0).wait()
                weight_copy(static, p, 1).wait()

            both_phases(phase, waits)

        slot = i - phase * per_phase
        x = normed[phase, block]
        for which in range(2):
            product = jnp.dot(x, w_in[phase, p, which], preferred_element_type=jnp.float32)
            own[slot, 0, which] = product[:half_rows]
            own[slot, 1, which] = product[half_rows:]

    def forward(d):
        def body(i, phase, block, p):
            slot = i - phase * per_phase
            pb = phase * blocks + block

            @pl.when(place[d] == 0)
            def _():
                part_out[i, d] = own[slot, d].astype(jnp.bfloat16)
                part_copy(d, i).start()

                @pl.when(p == 0)
                def _():
                    sq_out[pb, d] = sq_own[phase, block, d]
                    square_copy(d, pb).start()

            @pl.when((place[d] > 0) & (place[d] < R - 1))
            def _():
                part_copy(d, i).wait_recv()
                part_out[i, d] = (own[slot, d] + part_in[i, d].astype(jnp.float32)).astype(
                    jnp.bfloat16
                )
                part_copy(d, i).start()

                @pl.when(p == 0)
                def _():
                    square_copy(d, pb).wait_recv()
                    sq_out[pb, d] = sq_own[phase, block, d] + sq_in[pb, d]
                    square_copy(d, pb).start()

            @pl.when(place[d] == R - 1)
            def _():
                @pl.when(p == 0)
                def _():
                    square_copy(d, pb).wait_recv()
                    mean = (sq_own[phase, block, d] + sq_in[pb, d])[:1] / model
                    line = lax.rsqrt(mean + epsilon)
                    column = jnp.sum(jnp.where(diagonal(), line, 0.0), axis=1, keepdims=True)
                    scale[d] = jnp.broadcast_to(column, (half_rows, LANES))

                part_copy(d, i).wait_recv()
                factor = scale[d][:, :1]
                gate = (own[slot, d, 0] + part_in[i, d, 0].astype(jnp.float32)) * factor
                up = (own[slot, d, 1] + part_in[i, d, 1].astype(jnp.float32)) * factor
                hidden[i, d] = (gate / (1.0 + jnp.exp(-gate)) * up).astype(jnp.bfloat16)
                hidden_copy(d, i).start()

        return body

    def pass_back(d):
        def body(i, phase, block, p):
            @pl.when(place[d] < R - 1)
            def _():
                hidden_copy(d, i).wait_recv()

                @pl.when(place[d] > 0)
                def _():
                    hidden_copy(d, i).start()

        return body

    def down(i, phase, block, p):
        @pl.when(block == 0)
        def _():
            both_phases(phase, lambda static: weight_copy(static, p, 2).wait())

        product = jnp.dot(
            hidden[i].reshape(rows, width), w_down[phase, p], preferred_element_type=jnp.float32
        ).reshape(total.shape)

        @pl.when(p == 0)
        def _():
            total[...] = product

        @pl.when(p > 0)
        def _():
            total[...] += product

        @pl.when(p == pieces - 1)
        def _():
            pb = phase * blocks + block
            rs_own[pb] = total[c]
            rs_out[pb] = total[...].astype(jnp.bfloat16)
            for k in range(1, C):
                reduce_copy(pb, k).start()

    def reduce(i, phase, block, p):
        @pl.when(p == pieces - 1)
        def _():
            pb = phase * blocks + block
            branch = rs_own[pb]
            for k in range(1, C):
                reduce_copy(pb, k).wait_recv()
                branch = branch + rs_in[pb, k - 1].astype(jnp.float32)

            @pl.when(phase == 0)
            def _():
                values = residual[block, c].astype(jnp.float32)
                merged[pb, c] = (values + 0.5 * branch).astype(jnp.bfloat16)

            @pl.when(phase == 1)
            def _():
                values = merged[block, c].astype(jnp.float32)
                merged[pb, c] = (values + 0.5 * branch).astype(jnp.bfloat16)

            for k in range(1, C):
                spread_copy(pb, k).start()

    def spread(i, phase, block, p):
        @pl.when(p == pieces - 1)
        def _():
            pb = phase * blocks + block
            for k in range(1, C):
                spread_copy(pb, k).wait_recv()

            @pl.when(phase == 0)
            def _():
                prepare(1, block, merged[pb].reshape(rows, -1), gain_second)

            @pl.when(phase == 1)
            def _():
                out[block] = merged[pb]

    reach = HOP * (R - 1)
    end = 2 * reach

    def step(s, carry):
        load_rest(s)
        for d in range(2):
            at_step(s - 1 - HOP * place[d], forward(d))
        for d in range(2):
            at_step(s - 1 - reach - HOP * (R - 1 - place[d]), pass_back(d))
        at_step(s - 1 - end, down)
        at_step(s - 1 - end - REDUCE, reduce)
        at_step(s - 1 - end - REDUCE - SPREAD, spread)

        @pl.when(s + 1 < blocks)
        def _():
            first(s + 1)

        at_step(s, project)
        return carry

    lax.fori_loop(0, count + gap + end + REDUCE + SPREAD + 1, step, 0)

    def finish(i, carry):
        for d in range(2):

            @pl.when(place[d] < R - 1)
            def _():
                part_copy(d, i).wait_send()

            @pl.when(place[d] > 0)
            def _():
                hidden_copy(d, i).wait_send()

        return carry

    lax.fori_loop(0, count, finish, 0)

    def finish_block(pb, carry):
        for d in range(2):

            @pl.when(place[d] < R - 1)
            def _():
                square_copy(d, pb).wait_send()

        for k in range(1, C):
            reduce_copy(pb, k).wait_send()
            spread_copy(pb, k).wait_send()
        return carry

    lax.fori_loop(0, 2 * blocks, finish_block, 0)


def solution(mesh):
    R, C = mesh.shape["ra"], mesh.shape["cb"]

    def per_device(
        residual,
        gain_first,
        gate_first,
        up_first,
        down_first,
        gain_second,
        gate_second,
        up_second,
        down_second,
    ):
        tokens, depth = residual.shape
        units = gate_first.shape[1]
        blocks = max(1, min(4, tokens // (16 * C)))
        width = 2 * LANES if units % (2 * LANES) == 0 else units
        pieces = units // width
        rows = tokens // blocks
        half_rows = rows // 2
        share = rows // C
        count = 2 * blocks * pieces
        end = 1 + 2 * HOP * (R - 1) + REDUCE + SPREAD
        gap = max(0, pieces - 1 + end - blocks * pieces)
        bf16, f32 = jnp.bfloat16, jnp.float32
        vmem = functools.partial(pl.BlockSpec, memory_space=pltpu.VMEM)
        hbm = functools.partial(pl.BlockSpec, memory_space=pl.ANY)
        pbs = 2 * blocks
        dma = pltpu.SemaphoreType.DMA
        result = pl.pallas_call(
            functools.partial(
                kernel, (R, C, blocks, pieces, width, half_rows, gap, float(depth * R))
            ),
            out_shape=jax.ShapeDtypeStruct((blocks, C, share, depth), bf16),
            in_specs=[vmem()] * 3 + [hbm()] * 6,
            out_specs=vmem(),
            scratch_shapes=[
                pltpu.VMEM((2, pieces, 2, depth, width), bf16),
                pltpu.VMEM((2, pieces, width, depth), bf16),
                pltpu.VMEM((2, blocks, rows, depth), bf16),
                pltpu.VMEM((blocks * pieces, 2, 2, half_rows, width), f32),
                pltpu.VMEM((count, 2, 2, half_rows, width), bf16),
                pltpu.VMEM((count, 2, 2, half_rows, width), bf16),
                pltpu.VMEM((count, 2, half_rows, width), bf16),
                pltpu.VMEM((C, share, depth), f32),
                pltpu.VMEM((pbs, share, depth), f32),
                pltpu.VMEM((pbs, C, share, depth), bf16),
                pltpu.VMEM((pbs, C - 1, share, depth), bf16),
                pltpu.VMEM((pbs, C, share, depth), bf16),
                pltpu.VMEM((2, blocks, 2, TILE, half_rows), f32),
                pltpu.VMEM((pbs, 2, TILE, half_rows), f32),
                pltpu.VMEM((pbs, 2, TILE, half_rows), f32),
                pltpu.VMEM((2, half_rows, LANES), f32),
                dma((2, 3, pieces)),
                dma((2, count)),
                dma((2, count)),
                dma((2, count)),
                dma((2, count)),
                dma((2, pbs)),
                dma((2, pbs)),
                dma((pbs, C - 1)),
                dma((pbs, C - 1)),
                dma((pbs, C - 1)),
                dma((pbs, C - 1)),
            ],
            compiler_params=pltpu.CompilerParams(
                collective_id=0, has_side_effects=True, vmem_limit_bytes=67043328
            ),
        )(
            residual.reshape(blocks, C, share, depth),
            gain_first.reshape(1, depth),
            gain_second.reshape(1, depth),
            gate_first,
            up_first,
            down_first,
            gate_second,
            up_second,
            down_second,
        )
        return result.reshape(tokens, depth)

    in_specs = (
        P("grp", "ra"),
        P("ra"),
        P("ra", "cb"),
        P("ra", "cb"),
        P("cb", "ra"),
        P("ra"),
        P("ra", "cb"),
        P("ra", "cb"),
        P("cb", "ra"),
    )
    return jax.shard_map(
        per_device, mesh=mesh, in_specs=in_specs, out_specs=P("grp", "ra"), check_vma=False
    )
```
